32 devices in a mesh: ep: 8 (over z, x), tp: 4 (over y, core).
Axes of the slice: x: 2, y: 2, z: 4, core: 2. Of those that a mesh axis runs over, the one named last changes fastest.
Arguments:
- queries: bfloat16 [12288, 1024], P(('ep', 'tp')), may hold values from -250 to 250
- keys_values: bfloat16 [2, 12288, 256], P(None, ('ep', 'tp')), may hold values from -8 to 8
- sink_logits: float32 [16], replicated, may hold values from 2 to 6
- moe_rows: bfloat16 [2048, 2048], P('ep'), may hold values from -600 to 600
- norm_gain: float32 [2048], replicated, may hold values from 0.1 to 1.9
- group_choice: int32 [2048], P('ep'), may hold values from 0 to 1, as said below
- member_choice: int32 [2048, 2], P('ep'), may hold values from 0 to 3, as said below
- route_weight: float32 [2048, 2], P('ep'), may hold values from 0.1 to 1
- w_gate: bfloat16 [8, 2048, 2048], P('ep', None, 'tp'), may hold values from -0.125 to 0.125
- w_up: bfloat16 [8, 2048, 2048], P('ep', None, 'tp'), may hold values from -0.125 to 0.125
- w_down: bfloat16 [8, 2048, 2048], P('ep', None, 'tp'), may hold values from -0.125 to 0.125
Outputs:
- attended: bfloat16 [12288, 1024], P(('ep', 'tp'))
- mixed: bfloat16 [2048, 2048], P('ep', 'tp')
The draws below stay inside these ranges and needn't reach their ends.
Inputs may be any that keep to these rules, and one draw needn't show every extreme that they name: With expert = group_choice * 4 + member_choice, within the 256 rows of one index of ep no expert is named by more than 128 rows, and some expert is named by exactly 128 rows. `member_choice`: the 2 entries of a row differ.
All inputs are finite; a program needn't handle non-finite values.
Results may differ from the reference program's by a relative error of at most 0.007.
Values may be sent and summed in bfloat16 or wider, within the bound.
A program may use at most 64 MiB of HBM per device.

```python
import math
import jax
import jax.numpy as jnp
from jax import lax

D = 2048
QH = 16
KVH = 4
HD = 64
WINDOW = 128
MOE_ROWS = 256
FF = 2048
EPG = 4
TOP = 2
EXPERTS = 8
ATOKENS = 12288
MOE_TOKENS = 2048
CAP = 128
N_EP = 8


def attention_pair(key):
    base_key = jax.random.fold_in(key, 101)
    seed_query, seed_keys, seed_value = jax.random.split(base_key, 3)
    queries = 1.5 * jax.random.normal(seed_query, (ATOKENS, QH * HD), jnp.float32)
    key_rows = jax.random.normal(seed_keys, (ATOKENS, KVH, HD), jnp.float32)
    values = 2.0 * jax.random.normal(seed_value, (ATOKENS, KVH * HD), jnp.float32)
    queries = jnp.clip(queries, -250.0, 250.0)
    stacked = jnp.clip(jnp.stack([key_rows.reshape(ATOKENS, KVH * HD), values]), -8.0, 8.0)
    return (queries.astype(jnp.bfloat16), stacked.astype(jnp.bfloat16))


def draw_queries(key, part):
    return attention_pair(key)[0]


def draw_keys_values(key, part):
    return attention_pair(key)[1]


def draw_moe_rows(key, part):
    base_key = jax.random.fold_in(key, 202)
    seed_rows, seed_columns, seed_noise = jax.random.split(base_key, 3)
    row_scale = jnp.exp(jax.random.uniform(seed_rows, (MOE_TOKENS, 1), jnp.float32, 0.0, math.log(10.0)))
    column_scale = jnp.exp(jax.random.uniform(seed_columns, (1, D), jnp.float32, 0.0, math.log(10.0)))
    values = row_scale * column_scale * jax.random.normal(seed_noise, (MOE_TOKENS, D), jnp.float32)
    return jnp.clip(values, -600.0, 600.0).astype(jnp.bfloat16)


def route_pair(key):
    base_key = jax.random.fold_in(key, 303)
    groups = EXPERTS // EPG
    seat_count = CAP * EPG // TOP
    star_rows = (CAP - 1) * EPG // TOP + 1
    others = MOE_ROWS - star_rows
    blocks = MOE_TOKENS // MOE_ROWS
    seed_star, seed_order, seed_blocks = jax.random.split(base_key, 3)
    star_group = jax.random.randint(seed_star, (), 0, groups)
    star_order = jax.random.permutation(seed_order, EPG)

    def one_block(block_key):
        seed_seat, seed_perm, seed_shuffle = jax.random.split(block_key, 3)
        seat_order = jax.random.permutation(seed_seat, (groups - 1) * seat_count)[:others]
        other_group = seat_order // seat_count
        other_group = other_group + (other_group >= star_group).astype(jnp.int32)
        group_all = jnp.concatenate([jnp.full((star_rows,), star_group, jnp.int32), other_group.astype(jnp.int32)])
        slot_all = jnp.concatenate([jnp.arange(star_rows, dtype=jnp.int32), (seat_order % seat_count).astype(jnp.int32)])
        orders = jax.vmap(lambda seed_one: jax.random.permutation(seed_one, EPG))(jax.random.split(seed_perm, groups))
        orders = jnp.where((jnp.arange(groups) == star_group)[:, None], star_order[None, :], orders)
        columns = (TOP * slot_all[:, None] + jnp.arange(TOP, dtype=jnp.int32)[None, :]) % EPG
        members = orders[group_all[:, None], columns]
        shuffle = jax.random.permutation(seed_shuffle, MOE_ROWS)
        return (group_all[shuffle], members[shuffle])
    group_out, member_out = jax.vmap(one_block)(jax.random.split(seed_blocks, blocks))
    return (group_out.reshape(MOE_TOKENS).astype(jnp.int32), member_out.reshape(MOE_TOKENS, TOP).astype(jnp.int32))


def draw_group_choice(key, part):
    return route_pair(key)[0]


def draw_member_choice(key, part):
    return route_pair(key)[1]


def level_of(key, extent, pieces, least, high):
    loudness = 1.0
    for dim, shards_of in pieces:
        steps = jax.random.uniform(jax.random.fold_in(jax.random.fold_in(key, 6), dim), (shards_of,), jnp.float32, least / len(pieces), high / len(pieces))
        loudness = loudness * jnp.repeat(jnp.exp(steps), extent[dim] // shards_of).reshape((-1,) + (1,) * (len(extent) - 1 - dim))
    return loudness


def bell_draw(key, dims, scale, limit, cuts=(), kind=jnp.bfloat16):
    values = jax.random.normal(key, dims, jnp.float32) * scale
    if len(cuts) > 0:
        values = level_of(key, dims, cuts, -0.22, 0.18) * values
    return jnp.clip(values, min=-limit, max=limit).astype(kind)


def setup_inputs(seed: int = 0) -> dict:
    keys = jax.random.split(jax.random.key(seed), 12)
    queries = draw_queries(jax.random.fold_in(keys[11], 71), 0)
    keys_values = draw_keys_values(jax.random.fold_in(keys[11], 71), 0)
    sink_logits = jnp.clip(jax.random.uniform(keys[2], (QH,), jnp.float32, 2.0, 6.0), 2.0, 6.0)
    moe_rows = draw_moe_rows(jax.random.fold_in(keys[11], 71), 0)
    norm_gain = jnp.clip(1.0 + 0.18 * jax.random.normal(keys[4], (D,), jnp.float32), 0.1, 1.9)
    group_choice = draw_group_choice(jax.random.fold_in(keys[11], 71), 0)
    member_choice = draw_member_choice(jax.random.fold_in(keys[11], 71), 0)
    route_weight = jnp.clip(0.1 + 0.9 * jax.random.uniform(keys[7], (MOE_TOKENS, TOP), jnp.float32) ** level_of(keys[7], (MOE_TOKENS, TOP), ((0, 8),), -0.2, 0.2), 0.1, 1.0)
    w_gate = bell_draw(keys[8], (EXPERTS, D, FF), D ** -0.5, 0.125, ((0, 8), (2, 4)))
    w_up = bell_draw(keys[9], (EXPERTS, D, FF), D ** -0.5, 0.125, ((0, 8), (2, 4)))
    w_down = bell_draw(keys[10], (EXPERTS, FF, D), FF ** -0.5, 0.125, ((0, 8), (2, 4)))
    return {"queries": queries, "keys_values": keys_values, "sink_logits": sink_logits, "moe_rows": moe_rows, "norm_gain": norm_gain, "group_choice": group_choice, "member_choice": member_choice, "route_weight": route_weight, "w_gate": w_gate, "w_up": w_up, "w_down": w_down}


def attend_all(queries, keys_values, sink_logits):
    sharing = QH // KVH
    blocks = ATOKENS // WINDOW
    padded = jnp.pad(keys_values, ((0, 0), (WINDOW, 0), (0, 0)))
    first_half = padded[:, :ATOKENS].reshape(2, blocks, WINDOW, KVH, HD)
    second_half = padded[:, WINDOW:].reshape(2, blocks, WINDOW, KVH, HD)
    banded = jnp.concatenate([first_half, second_half], axis=2)
    query_blocks = queries.reshape(blocks, WINDOW, KVH, sharing, HD)
    key_column = jnp.arange(2 * WINDOW, dtype=jnp.int32)
    distance = jnp.arange(WINDOW, dtype=jnp.int32)[:, None] + WINDOW - key_column[None, :]
    inside = (distance >= 0) & (distance < WINDOW)
    sink_column = sink_logits.reshape(KVH, sharing)[:, :, None]

    def one_block(operands):
        query_block, key_block, value_block, number = operands
        scores = jnp.einsum('qhgd,khd->hgqk', query_block.astype(jnp.float32), key_block.astype(jnp.float32)) * HD ** (-0.5)
        visible = inside & (number * WINDOW + key_column[None, :] - WINDOW >= 0)
        scores = jnp.where(visible[None, None], scores, -1e+30)
        highest = jnp.maximum(lax.optimization_barrier(jnp.max(scores, axis=-1)), sink_column)
        weights = jnp.exp(scores - highest[..., None])
        totals = lax.optimization_barrier(jnp.sum(weights, axis=-1)) + jnp.exp(sink_column - highest)
        rounded = lax.optimization_barrier(weights.astype(jnp.bfloat16)).astype(jnp.float32)
        summed = jnp.einsum('hgqk,khd->qhgd', rounded, value_block.astype(jnp.float32))
        return (summed / jnp.transpose(totals, (2, 0, 1))[..., None]).astype(jnp.bfloat16)
    result = lax.map(one_block, (query_blocks, banded[0], banded[1], jnp.arange(blocks, dtype=jnp.int32)))
    return result.reshape(ATOKENS, QH * HD)

def experts_all(moe_rows, norm_gain, group_choice, member_choice, route_weight, w_gate, w_up, w_down):
    values = moe_rows.astype(jnp.float32)
    normed = (values * lax.rsqrt(lax.optimization_barrier(jnp.mean(values * values, axis=1, keepdims=True)) + 1e-06) * norm_gain).astype(jnp.bfloat16)
    chosen = (group_choice[:, None] * EPG + member_choice).astype(jnp.int32).reshape(N_EP, MOE_ROWS * TOP)
    onehot = (chosen[:, :, None] == jnp.arange(EXPERTS, dtype=jnp.int32)[None, None, :]).astype(jnp.int32)
    earlier = (jnp.cumsum(onehot, axis=1) - onehot).astype(jnp.int32)
    position = lax.optimization_barrier(jnp.sum(earlier * onehot, axis=2)).astype(jnp.int32)
    source = jnp.arange(N_EP, dtype=jnp.int32)[:, None]
    placed = (chosen * (N_EP * CAP) + source * CAP + position).astype(jnp.int32).reshape(MOE_TOKENS, TOP)
    source_row = jnp.arange(MOE_TOKENS * TOP, dtype=jnp.int32) // TOP
    lookup = jnp.full((EXPERTS * N_EP * CAP,), MOE_TOKENS, jnp.int32).at[placed.reshape(-1)].set(source_row)
    padded = jnp.concatenate([normed, jnp.zeros((1, D), jnp.bfloat16)], axis=0)

    def one_expert(operands):
        row_index, gate_weight, up_weight, down_weight = operands
        inputs = padded[row_index]
        gate_part = jnp.dot(inputs, gate_weight, preferred_element_type=jnp.float32)
        up_part = jnp.dot(inputs, up_weight, preferred_element_type=jnp.float32)
        hidden = (jax.nn.silu(gate_part) * up_part).astype(jnp.bfloat16)
        return jnp.dot(hidden, down_weight, preferred_element_type=jnp.float32).astype(jnp.bfloat16)
    produced = lax.map(one_expert, (lookup.reshape(EXPERTS, N_EP * CAP), w_gate, w_up, w_down))
    picked = produced.reshape(EXPERTS * N_EP * CAP, D)[placed].astype(jnp.float32)
    return lax.optimization_barrier(jnp.sum(route_weight[:, :, None] * picked, axis=1)).astype(jnp.bfloat16)

def reference(queries, keys_values, sink_logits, moe_rows, norm_gain, group_choice, member_choice, route_weight, w_gate, w_up, w_down):
    attended = attend_all(queries, keys_values, sink_logits)
    mixed = experts_all(moe_rows, norm_gain, group_choice, member_choice, route_weight, w_gate, w_up, w_down)
    return (attended, mixed)
```

```python
import functools

import jax
import jax.numpy as jnp
from jax import lax
from jax.experimental import pallas as pl
from jax.experimental.pallas import tpu as pltpu
from jax.sharding import PartitionSpec as P

QH = 16
KVH = 4
HD = 64
WINDOW = 128
EPG = 4
TOP = 2
CORES = 2
WIDE = 4
RAWAT = 2
LAG = 6
MESH = pl.DeviceIdType.MESH
F32 = jnp.float32
BF16 = jnp.bfloat16


def kernel(
    n, tp, cap,
    q_hbm, kv_hbm, sink_ref, rows_hbm, gain_ref, group_ref, member_ref, rw_ref,
    wg_hbm, wu_hbm, wd_hbm,
    att_ref, mix_ref,
    wg, wu, wd, q, rows, kvj, nrm, raw, posm, S, SN, X, H, O, R, acc, line, col,
    loc, edge_s, edge_r, raw_s, raw_r, pos_s, pos_r, s_s, r1, x_s, x2, x3, h_s, h2, h3, o_s, o_r,
):
    e = lax.axis_index("ep")
    t = lax.axis_index("tp")
    ny = tp // CORES
    y = t // CORES
    core = lax.rem(t, CORES)
    mate = y * CORES + (1 - core)
    near = min(EPG, n)
    sides = n // near
    wide = min(WIDE, near)
    tokens, width = rows.shape
    dc = width // tp
    ffs = wg.shape[1]
    length = q.shape[0]
    lin = e * tp + t
    total = n * tp
    after = lax.rem(lin + 1, total)
    before = lax.rem(lin + total - 1, total)
    home = core * ny
    own = home + y

    def block_of(k):
        return (k % CORES) * ny + k // CORES

    def partner(m):
        out = 0
        bit = 1
        while bit < n:
            out = out + bit * lax.rem(e // bit + m // bit, 2)
            bit *= 2
        return out

    def ypeer(j):
        return lax.rem(y + j, ny) * CORES + core

    barrier = pltpu.get_barrier_semaphore()

    def greet(m, _):
        pl.semaphore_signal(barrier, inc=1, device_id=(partner(m), t), device_id_type=MESH)
        return 0

    lax.fori_loop(1, n, greet, 0)
    for j in range(1, ny):
        pl.semaphore_signal(barrier, inc=1, device_id=(e, ypeer(j)), device_id_type=MESH)
    pl.semaphore_signal(barrier, inc=1, device_id=(e, mate), device_id_type=MESH)
    for lin2 in (after, before):
        pl.semaphore_signal(
            barrier, inc=1, device_id=(lin2 // tp, lax.rem(lin2, tp)), device_id_type=MESH
        )

    loads = [
        pltpu.make_async_copy(rows_hbm, rows, loc.at[0]),
        pltpu.make_async_copy(wg_hbm.at[0], wg, loc.at[1]),
        pltpu.make_async_copy(wu_hbm.at[0], wu, loc.at[2]),
        pltpu.make_async_copy(q_hbm, q, loc.at[3]),
        pltpu.make_async_copy(kv_hbm, kvj.at[:, pl.ds(WINDOW, length)], loc.at[4]),
        pltpu.make_async_copy(wd_hbm.at[0], wd, loc.at[5]),
    ]
    loads[0].start()

    a_i = lax.broadcasted_iota(jnp.int32, (tokens, tokens), 0)
    b_i = lax.broadcasted_iota(jnp.int32, (tokens, tokens), 1)
    erow = lax.broadcasted_iota(jnp.int32, (n, tokens), 0)
    e0 = group_ref[...] * EPG + member_ref[0:1, :]
    e1 = group_ref[...] * EPG + member_ref[1:2, :]
    named = (e0 == erow) | (e1 == erow)
    upper = (a_i < b_i).astype(F32).astype(BF16)
    pos = jnp.dot(named.astype(F32).astype(BF16), upper, preferred_element_type=F32)
    posm[0] = jnp.where(named, pos, -1.0).astype(jnp.int32)
    line[0:1, :] = e0.astype(F32)
    line[1:2, :] = e1.astype(F32)
    line[2:3, :] = jnp.sum(jnp.where(e0 == erow, pos, 0.0), axis=0, keepdims=True)
    line[3:4, :] = jnp.sum(jnp.where(e1 == erow, pos, 0.0), axis=0, keepdims=True)
    line[4:6, :] = rw_ref[...]
    line[6:, :] = jnp.zeros((122, tokens), F32)
    col[...] = line[...].T
    acc[...] = jnp.zeros_like(acc)

    @pl.when(lin == 0)
    def _():
        kvj[:, 0:WINDOW, :] = jnp.zeros((2, WINDOW, kvj.shape[2]), BF16)

    chunk = 32

    def norm_rows(r, _):
        at = pl.ds(pl.multiple_of(r * chunk, chunk), chunk)
        v = rows[at, :].astype(F32)
        m = jnp.mean(v * v, axis=1, keepdims=True)
        nv = (v * lax.rsqrt(m + 1e-06) * gain_ref[...]).astype(BF16)
        for k in range(tp):
            nrm[block_of(k), at, :] = nv[:, k * dc : (k + 1) * dc]
        return 0

    loads[0].wait()
    for c in loads[1:]:
        c.start()
    with jax.named_scope("norm"):
        lax.fori_loop(0, tokens // chunk, norm_rows, 0)

    def slots_of(side, x):
        slot = lax.broadcasted_iota(jnp.int32, (cap, tokens), 0)
        return (posm[side, pl.ds(x, 1), :] == slot).astype(F32).astype(BF16)

    def gathered(slots, rows_of):
        return jnp.dot(slots, rows_of, preferred_element_type=F32).astype(BF16)

    edge = pltpu.make_async_remote_copy(
        src_ref=kv_hbm.at[:, pl.ds(length - WINDOW, WINDOW)], dst_ref=kvj.at[:, pl.ds(0, WINDOW)],
        send_sem=edge_s, recv_sem=edge_r,
        device_id=(after // tp, lax.rem(after, tp)), device_id_type=MESH,
    )

    def send_rows(m):
        pltpu.make_async_remote_copy(
            src_ref=S.at[m], dst_ref=X.at[m, own], send_sem=s_s.at[m], recv_sem=r1.at[m],
            device_id=(partner(lax.rem(m, near)), t), device_id_type=MESH,
        ).start()

    def send_near(m):
        slots = slots_of(0, partner(m))
        if m < wide:
            for j in range(ny):
                SN[m, j] = gathered(slots, nrm[home + j])
            pltpu.make_async_remote_copy(
                src_ref=SN.at[m], dst_ref=X.at[m, pl.ds(home, ny)], send_sem=s_s.at[m],
                recv_sem=r1.at[m], device_id=(partner(m), t), device_id_type=MESH,
            ).start()
        else:
            S[m] = gathered(slots, nrm[own])
            send_rows(m)

    def send_raw(g, _):
        to = (partner(g * near), t)
        pltpu.make_async_remote_copy(
            src_ref=posm.at[0], dst_ref=posm.at[g], send_sem=pos_s.at[g], recv_sem=pos_r.at[g],
            device_id=to, device_id_type=MESH,
        ).start()
        pltpu.make_async_remote_copy(
            src_ref=nrm.at[own], dst_ref=raw.at[g], send_sem=raw_s.at[g], recv_sem=raw_r.at[g],
            device_id=to, device_id_type=MESH,
        ).start()
        return 0

    with jax.named_scope("barrier"):
        pl.semaphore_wait(barrier, (n - 1) + (ny - 1) + 1 + 2)
    with jax.named_scope("build"):
        first_near = near // 2
        send_near(first_near)
        lax.fori_loop(1, sides, send_raw, 0)
        for m in range(1, near - 1):
            if m != first_near:
                send_near(m)

    @pl.when(lin < total - 1)
    def _():
        edge.start()

    mine = slots_of(0, e)
    for k in range(tp):
        X[0, k] = gathered(mine, nrm[k])

    def expect(ref, sem):
        pltpu.make_async_copy(ref, ref, sem).wait()

    def spread(buf, m, sends, to_y):
        for j in range(1, ny):
            pltpu.make_async_remote_copy(
                src_ref=buf.at[m, own], dst_ref=buf.at[m, own], send_sem=sends.at[m],
                recv_sem=to_y.at[m], device_id=(e, ypeer(j)), device_id_type=MESH,
            ).start()

    def relay(buf, m, sends, to_mate):
        half = buf.at[m, pl.ds(home, ny)]
        pltpu.make_async_remote_copy(
            src_ref=half, dst_ref=half, send_sem=sends.at[m],
            recv_sem=to_mate.at[m], device_id=(e, mate), device_id_type=MESH,
        ).start()

    def gate_up(m):
        x = jnp.concatenate([X[m, block_of(k)] for k in range(tp)], axis=1)
        step = min(256, ffs)
        for c in range(0, ffs, step):
            g = jnp.dot(x, wg[:, c : c + step], preferred_element_type=F32)
            u = jnp.dot(x, wu[:, c : c + step], preferred_element_type=F32)
            H[m, own, :, c : c + step] = (g / (1.0 + jnp.exp(-g)) * u).astype(BF16)

    def down(m):
        h = jnp.concatenate([H[m, block_of(k)] for k in range(tp)], axis=1)
        O[m] = jnp.dot(h, wd[...], preferred_element_type=F32).astype(BF16)

    def combine(m, ref):
        x = partner(m)
        first = col[:, 0:1] == x.astype(F32)
        second = col[:, 1:2] == x.astype(F32)
        where = jnp.where(first, col[:, 2:3], jnp.where(second, col[:, 3:4], -1.0))
        weight = jnp.where(first, col[:, 4:5], jnp.where(second, col[:, 5:6], 0.0))
        slot = lax.broadcasted_iota(jnp.int32, (tokens, cap), 1).astype(F32)
        pick = (where == slot).astype(F32).astype(BF16)
        acc[...] += weight * jnp.dot(pick, ref[m], preferred_element_type=F32)

    sharing = QH // KVH

    def attend(b, half):
        base = pl.multiple_of(b * WINDOW, WINDOW)
        qi = lax.broadcasted_iota(jnp.int32, (WINDOW, 2 * WINDOW), 0)
        kj = lax.broadcasted_iota(jnp.int32, (WINDOW, 2 * WINDOW), 1)
        dist = qi + WINDOW - kj
        seen = (dist >= 0) & (dist < WINDOW) & (lin * length + base + kj - WINDOW >= 0)
        for pair in range(half * QH // 4, (half + 1) * QH // 4):
            h = 2 * pair // sharing
            lo = (h // 2) * 128
            keys = kvj[0, pl.ds(base, 2 * WINDOW), lo : lo + 128]
            vals = kvj[1, pl.ds(base, 2 * WINDOW), lo : lo + 128]
            off = (h % 2) * HD
            keys = keys[:, off : off + HD]
            vals = vals[:, off : off + HD]
            qp = q[pl.ds(base, WINDOW), pair * 128 : (pair + 1) * 128]
            outs = []
            for g in range(2):
                s = lax.dot_general(
                    qp[:, g * HD : (g + 1) * HD], keys, (((1,), (1,)), ((), ())),
                    preferred_element_type=F32,
                ) * HD ** (-0.5)
                s = jnp.where(seen, s, -1e30)
                sink = sink_ref[2 * pair + g]
                top = jnp.maximum(jnp.max(s, axis=1, keepdims=True), sink)
                w = jnp.exp(s - top)
                tot = jnp.sum(w, axis=1, keepdims=True) + jnp.exp(sink - top)
                o = jnp.dot(w.astype(BF16), vals, preferred_element_type=F32)
                outs.append((o / tot).astype(BF16))
            att_ref[pl.ds(base, WINDOW), pair * 128 : (pair + 1) * 128] = jnp.concatenate(outs, axis=1)

    order = [0, *range(1, near - 1), *range(near, n), near - 1]

    def chosen(i):
        m = order[0]
        for j in range(1, n):
            m = jnp.where(i >= j, order[j], m)
        return m

    blocks = length // WINDOW
    units = 2 * blocks

    def take_raw(g):
        m = g * near
        with jax.named_scope("w_raw"):
            expect(posm.at[g], pos_r.at[g])
            expect(raw.at[g], raw_r.at[g])
        with jax.named_scope("relay_rows"):
            for r in range(1, near):
                S[m + r] = gathered(slots_of(g, partner(r)), raw[g])
                send_rows(m + r)
            X[m, own] = gathered(slots_of(g, e), raw[g])
            spread(X, m, x_s, x2)

    def take(i):
        m = chosen(i)

        @pl.when((i < n) & (m >= wide) & (lax.rem(m, near) != 0))
        def _():
            with jax.named_scope("w_r1"):
                expect(X.at[m, own], r1.at[m])
            spread(X, m, x_s, x2)

    def fill(i):
        m = chosen(i)

        @pl.when((i < n) & (m >= wide))
        def _():
            with jax.named_scope("w_x2"):
                expect(X.at[m, pl.ds(0, ny - 1)], x2.at[m])
            relay(X, m, x_s, x3)

        @pl.when((i < n) & (m < wide))
        def _():
            with jax.named_scope("w_r1n"):
                expect(X.at[m, pl.ds(0, ny)], r1.at[m])
            relay(X, m, x_s, x3)

    loads[1].wait()
    loads[2].wait()

    def when_raw(i, mark):
        for g in range(1, sides):
            @pl.when(i == near * (g - 1) + mark)
            def _(g=g):
                take_raw(g)

    early = lax.rem(e // (near // 2), 2) == lax.rem(e // near, 2)

    def step(i, _):
        @pl.when(early)
        def _():
            when_raw(i, RAWAT)

        @pl.when(i >= 3)
        def _():
            take(i + 1)

        @pl.when(i > 0)
        def _():
            fill(i)

        @pl.when((i >= 3) & (i < 3))
        def _():
            take(i + 1)

        @pl.when(i < n)
        def _():
            m = chosen(i)

            @pl.when(i > 0)
            def _():
                with jax.named_scope("w_x3"):
                    expect(X.at[m, pl.ds(0, ny)], x3.at[m])

            with jax.named_scope("gate_up"):
                gate_up(m)
            spread(H, m, h_s, h2)

        @pl.when(i < 3)
        def _():
            take(i + 1)

        @pl.when(i == 0)
        def _():
            loads[3].wait()
            loads[4].wait()
            loads[5].wait()

        @pl.when(i == units - 2)
        def _():
            @pl.when(lin > 0)
            def _():
                with jax.named_scope("w_edge"):
                    edge.wait_recv()

        @pl.when(jnp.logical_not(early))
        def _():
            when_raw(i, RAWAT)

        @pl.when((i >= 1) & (i - 1 < n))
        def _():
            m = chosen(i - 1)
            with jax.named_scope("w_h2"):
                expect(H.at[m, pl.ds(0, ny - 1)], h2.at[m])
            relay(H, m, h_s, h3)

        for half in range(2):
            @pl.when((i < units) & (lax.rem(i, 2) == half))
            def _(half=half):
                with jax.named_scope("attend"):
                    attend(blocks - 1 - i // 2, half)

        @pl.when((i >= 1) & (i - 1 < n))
        def _():
            m = chosen(i - 1)
            with jax.named_scope("w_h3"):
                expect(H.at[m, pl.ds(0, ny)], h3.at[m])
            with jax.named_scope("down"):
                down(m)

            @pl.when(i > 1)
            def _():
                pltpu.make_async_remote_copy(
                    src_ref=O.at[m], dst_ref=R.at[m], send_sem=o_s.at[m], recv_sem=o_r.at[m],
                    device_id=(partner(m), t), device_id_type=MESH,
                ).start()

            @pl.when(i == 1)
            def _():
                combine(m, O)

        @pl.when(i == 3)
        def _():
            send_near(near - 1)

        @pl.when((i > LAG) & (i - LAG < n))
        def _():
            m = chosen(i - LAG)
            with jax.named_scope("w_o"):
                expect(R.at[m], o_r.at[m])
            with jax.named_scope("combine"):
                combine(m, R)

        return 0

    lax.fori_loop(0, n + LAG, step, 0)
    mix_ref[...] = acc[...].astype(BF16)

    def drain(m, _):
        @pl.when(m >= wide)
        def _():
            @pl.when(lax.rem(m, near) > 0)
            def _():
                expect(S.at[m], s_s.at[m])

            expect(X.at[m, pl.ds(0, 2 * ny - 1)], x_s.at[m])

        @pl.when((m > 0) & (m < wide))
        def _():
            expect(SN.at[m], s_s.at[m])
            expect(X.at[m, pl.ds(0, ny)], x_s.at[m])

        @pl.when(m > 0)
        def _():
            expect(O.at[m], o_s.at[m])

        @pl.when((m > 0) & (m < sides))
        def _():
            expect(posm.at[m], pos_s.at[m])
            expect(raw.at[m], raw_s.at[m])

        expect(H.at[m, pl.ds(0, 2 * ny - 1)], h_s.at[m])
        return 0

    with jax.named_scope("drain"):
        lax.fori_loop(0, n, drain, 0)

    @pl.when(lin < total - 1)
    def _():
        edge.wait_send()


def shards(
    queries, keys_values, sink_logits, moe_rows, norm_gain, group_choice, member_choice,
    route_weight, w_gate, w_up, w_down,
):
    n = lax.axis_size("ep")
    tp = lax.axis_size("tp")
    assert w_gate.shape[0] == 1
    tokens, width = moe_rows.shape
    cap = 2 * TOP * tokens // n
    ffs = w_gate.shape[2]
    out = w_down.shape[2]
    ff = w_down.shape[1]
    length = queries.shape[0]
    vmem = pl.BlockSpec(memory_space=pltpu.VMEM)
    anyspace = pl.BlockSpec(memory_space=pl.ANY)
    dma = pltpu.SemaphoreType.DMA
    return pl.pallas_call(
        functools.partial(kernel, n, tp, cap),
        out_shape=(
            pltpu.VMEM(queries.shape, BF16),
            pltpu.VMEM((tokens, out), BF16),
        ),
        in_specs=[
            anyspace, anyspace, pl.BlockSpec(memory_space=pltpu.SMEM), anyspace, vmem, vmem, vmem, vmem,
            anyspace, anyspace, anyspace,
        ],
        out_specs=(vmem, vmem),
        scratch_shapes=[
            pltpu.VMEM((width, ffs), BF16),
            pltpu.VMEM((width, ffs), BF16),
            pltpu.VMEM((ff, out), BF16),
            pltpu.VMEM(queries.shape, BF16),
            pltpu.VMEM(moe_rows.shape, BF16),
            pltpu.VMEM((2, WINDOW + length, keys_values.shape[2]), BF16),
            pltpu.VMEM((tp, tokens, width // tp), BF16),
            pltpu.VMEM((n // min(EPG, n), tokens, width // tp), BF16),
            pltpu.VMEM((n // min(EPG, n), n, tokens), jnp.int32),
            pltpu.VMEM((n, cap, width // tp), BF16),
            pltpu.VMEM((min(EPG, n), tp // CORES, cap, width // tp), BF16),
            pltpu.VMEM((n, tp, cap, width // tp), BF16),
            pltpu.VMEM((n, tp, cap, ffs), BF16),
            pltpu.VMEM((n, cap, out), BF16),
            pltpu.VMEM((n, cap, out), BF16),
            pltpu.VMEM((tokens, out), F32),
            pltpu.VMEM((128, tokens), F32),
            pltpu.VMEM((tokens, 128), F32),
            dma((6,)), dma, dma,
            dma((n // min(EPG, n),)), dma((n // min(EPG, n),)), dma((n // min(EPG, n),)), dma((n // min(EPG, n),)),
            dma((n,)), dma((n,)), dma((n,)), dma((n,)), dma((n,)),
            dma((n,)), dma((n,)), dma((n,)), dma((n,)), dma((n,)),
        ],
        compiler_params=pltpu.CompilerParams(
            collective_id=0, has_side_effects=True, vmem_limit_bytes=56 * 1024 * 1024
        ),
    )(
        queries, keys_values, sink_logits, moe_rows, norm_gain.reshape(1, width),
        group_choice.reshape(1, tokens), member_choice.T, route_weight.T, w_gate, w_up, w_down,
    )


def solution(mesh):
    in_specs = (
        P(("ep", "tp"), None),
        P(None, ("ep", "tp"), None),
        P(),
        P("ep", None),
        P(),
        P("ep"),
        P("ep", None),
        P("ep", None),
        P("ep", None, "tp"),
        P("ep", None, "tp"),
        P("ep", None, "tp"),
    )
    out_specs = (P(("ep", "tp"), None), P("ep", "tp"))
    return jax.shard_map(shards, mesh=mesh, in_specs=in_specs, out_specs=out_specs, check_vma=False)
```

```python
import functools

import jax
import jax.numpy as jnp
from jax import lax
from jax.experimental import pallas as pl
from jax.experimental.pallas import tpu as pltpu
from jax.sharding import PartitionSpec as P

QH = 16
KVH = 4
HD = 64
WINDOW = 128
EPG = 4
TOP = 2
CORES = 2
ROW_PARTS = 4
WIDE = 4
RAWAT = 2
LAG = 6
MESH = pl.DeviceIdType.MESH
F32 = jnp.float32
BF16 = jnp.bfloat16


def kernel(
    n, tp, cap,
    q_hbm, kv_hbm, sink_hbm, rows_hbm, gain_hbm, group_hbm, member_hbm, rw_hbm,
    wg_hbm, wu_hbm, wd_hbm,
    att_ref, mix_ref,
    wg, wu, wd, q, rows, sink_ref, gain_ref, group_ref, member_ref, rw_ref, kvj, nrm, raw, posm, S, SN, X, H, O, R, acc, line, col,
    small, loc, edge_s, edge_r, raw_s, raw_r, pos_s, pos_r, s_s, r1, x_s, x2, x3, h_s, h2, h3, o_s, o_r,
):
    e = lax.axis_index("ep")
    t = lax.axis_index("tp")
    ny = tp // CORES
    y = t // CORES
    core = lax.rem(t, CORES)
    mate = y * CORES + (1 - core)
    near = min(EPG, n)
    sides = n // near
    wide = min(WIDE, near)
    tokens, width = rows.shape
    dc = width // tp
    ffs = wg.shape[1]
    length = q.shape[0]
    lin = e * tp + t
    total = n * tp
    after = lax.rem(lin + 1, total)
    before = lax.rem(lin + total - 1, total)
    home = core * ny
    own = home + y

    def block_of(k):
        return (k % CORES) * ny + k // CORES

    def partner(m):
        out = 0
        bit = 1
        while bit < n:
            out = out + bit * lax.rem(e // bit + m // bit, 2)
            bit *= 2
        return out

    def ypeer(j):
        return lax.rem(y + j, ny) * CORES + core

    barrier = pltpu.get_barrier_semaphore()

    def greet(m, _):
        pl.semaphore_signal(barrier, inc=1, device_id=(partner(m), t), device_id_type=MESH)
        return 0

    lax.fori_loop(1, n, greet, 0)
    for j in range(1, ny):
        pl.semaphore_signal(barrier, inc=1, device_id=(e, ypeer(j)), device_id_type=MESH)
    pl.semaphore_signal(barrier, inc=1, device_id=(e, mate), device_id_type=MESH)
    for lin2 in (after, before):
        pl.semaphore_signal(
            barrier, inc=1, device_id=(lin2 // tp, lax.rem(lin2, tp)), device_id_type=MESH
        )

    part = tokens // ROW_PARTS

    def row_load(k):
        at = pl.ds(k * part, part)
        return pltpu.make_async_copy(rows_hbm.at[at], rows.at[at], loc.at[k])

    row_loads = [row_load(k) for k in range(ROW_PARTS)]
    loads = [
        pltpu.make_async_copy(wg_hbm.at[0], wg, loc.at[ROW_PARTS + 0]),
        pltpu.make_async_copy(wu_hbm.at[0], wu, loc.at[ROW_PARTS + 1]),
        pltpu.make_async_copy(q_hbm, q, loc.at[ROW_PARTS + 2]),
        pltpu.make_async_copy(kv_hbm, kvj.at[:, pl.ds(WINDOW, length)], loc.at[ROW_PARTS + 3]),
        pltpu.make_async_copy(wd_hbm.at[0], wd, loc.at[ROW_PARTS + 4]),
    ]
    details = [
        pltpu.make_async_copy(a, b, small.at[i])
        for i, (a, b) in enumerate([
            (group_hbm, group_ref), (member_hbm, member_ref), (rw_hbm, rw_ref),
            (gain_hbm, gain_ref), (sink_hbm, sink_ref),
        ])
    ]
    for c in details[:3] + row_loads + details[3:]:
        c.start()

    for c in details[:3]:
        c.wait()
    a_i = lax.broadcasted_iota(jnp.int32, (tokens, tokens), 0)
    b_i = lax.broadcasted_iota(jnp.int32, (tokens, tokens), 1)
    erow = lax.broadcasted_iota(jnp.int32, (n, tokens), 0)
    e0 = group_ref[...] * EPG + member_ref[0:1, :]
    e1 = group_ref[...] * EPG + member_ref[1:2, :]
    named = (e0 == erow) | (e1 == erow)
    upper = (a_i < b_i).astype(F32).astype(BF16)
    pos = jnp.dot(named.astype(F32).astype(BF16), upper, preferred_element_type=F32)
    posm[0] = jnp.where(named, pos, -1.0).astype(jnp.int32)
    line[0:1, :] = e0.astype(F32)
    line[1:2, :] = e1.astype(F32)
    line[2:3, :] = jnp.sum(jnp.where(e0 == erow, pos, 0.0), axis=0, keepdims=True)
    line[3:4, :] = jnp.sum(jnp.where(e1 == erow, pos, 0.0), axis=0, keepdims=True)
    line[4:6, :] = rw_ref[...]
    line[6:, :] = jnp.zeros((122, tokens), F32)
    col[...] = line[...].T
    acc[...] = jnp.zeros_like(acc)

    @pl.when(lin == 0)
    def _():
        kvj[:, 0:WINDOW, :] = jnp.zeros((2, WINDOW, kvj.shape[2]), BF16)

    chunk = 32

    def norm_rows(r, _):
        at = pl.ds(pl.multiple_of(r * chunk, chunk), chunk)
        v = rows[at, :].astype(F32)
        m = jnp.mean(v * v, axis=1, keepdims=True)
        nv = (v * lax.rsqrt(m + 1e-06) * gain_ref[...]).astype(BF16)
        for k in range(tp):
            nrm[block_of(k), at, :] = nv[:, k * dc : (k + 1) * dc]
        return 0

    details[3].wait()
    for k in range(ROW_PARTS):
        row_loads[k].wait()
        if k == ROW_PARTS - 1:
            for c in loads:
                c.start()
        with jax.named_scope("norm"):
            lax.fori_loop(k * part // chunk, (k + 1) * part // chunk, norm_rows, 0, unroll=2)

    def slots_of(side, x):
        slot = lax.broadcasted_iota(jnp.int32, (cap, tokens), 0)
        return (posm[side, pl.ds(x, 1), :] == slot).astype(F32).astype(BF16)

    def gathered(slots, rows_of):
        return jnp.dot(slots, rows_of, preferred_element_type=F32).astype(BF16)

    edge = pltpu.make_async_remote_copy(
        src_ref=kv_hbm.at[:, pl.ds(length - WINDOW, WINDOW)], dst_ref=kvj.at[:, pl.ds(0, WINDOW)],
        send_sem=edge_s, recv_sem=edge_r,
        device_id=(after // tp, lax.rem(after, tp)), device_id_type=MESH,
    )

    def send_rows(m):
        pltpu.make_async_remote_copy(
            src_ref=S.at[m], dst_ref=X.at[m, own], send_sem=s_s.at[m], recv_sem=r1.at[m],
            device_id=(partner(lax.rem(m, near)), t), device_id_type=MESH,
        ).start()

    def send_near(m):
        slots = slots_of(0, partner(m))
        if m < wide:
            for j in range(ny):
                SN[m, j] = gathered(slots, nrm[home + j])
            pltpu.make_async_remote_copy(
                src_ref=SN.at[m], dst_ref=X.at[m, pl.ds(home, ny)], send_sem=s_s.at[m],
                recv_sem=r1.at[m], device_id=(partner(m), t), device_id_type=MESH,
            ).start()
        else:
            S[m] = gathered(slots, nrm[own])
            send_rows(m)

    def send_raw(g, _):
        to = (partner(g * near), t)
        pltpu.make_async_remote_copy(
            src_ref=posm.at[0], dst_ref=posm.at[g], send_sem=pos_s.at[g], recv_sem=pos_r.at[g],
            device_id=to, device_id_type=MESH,
        ).start()
        pltpu.make_async_remote_copy(
            src_ref=nrm.at[own], dst_ref=raw.at[g], send_sem=raw_s.at[g], recv_sem=raw_r.at[g],
            device_id=to, device_id_type=MESH,
        ).start()
        return 0

    with jax.named_scope("barrier"):
        pl.semaphore_wait(barrier, (n - 1) + (ny - 1) + 1 + 2)
    with jax.named_scope("build"):
        first_near = near // 2
        send_near(first_near)
        lax.fori_loop(1, sides, send_raw, 0)
        for m in range(1, near - 1):
            if m != first_near:
                send_near(m)

    @pl.when(lin < total - 1)
    def _():
        edge.start()

    mine = slots_of(0, e)
    for k in range(tp):
        X[0, k] = gathered(mine, nrm[k])

    def expect(ref, sem):
        pltpu.make_async_copy(ref, ref, sem).wait()

    def spread(buf, m, sends, to_y):
        for j in range(1, ny):
            pltpu.make_async_remote_copy(
                src_ref=buf.at[m, own], dst_ref=buf.at[m, own], send_sem=sends.at[m],
                recv_sem=to_y.at[m], device_id=(e, ypeer(j)), device_id_type=MESH,
            ).start()

    def relay(buf, m, sends, to_mate):
        half = buf.at[m, pl.ds(home, ny)]
        pltpu.make_async_remote_copy(
            src_ref=half, dst_ref=half, send_sem=sends.at[m],
            recv_sem=to_mate.at[m], device_id=(e, mate), device_id_type=MESH,
        ).start()

    def gate_up(m):
        x = jnp.concatenate([X[m, block_of(k)] for k in range(tp)], axis=1)
        step = min(256, ffs)
        for c in range(0, ffs, step):
            g = jnp.dot(x, wg[:, c : c + step], preferred_element_type=F32)
            u = jnp.dot(x, wu[:, c : c + step], preferred_element_type=F32)
            H[m, own, :, c : c + step] = (g / (1.0 + jnp.exp(-g)) * u).astype(BF16)

    def down(m):
        h = jnp.concatenate([H[m, block_of(k)] for k in range(tp)], axis=1)
        O[m] = jnp.dot(h, wd[...], preferred_element_type=F32).astype(BF16)

    def combine(m, ref):
        x = partner(m)
        first = col[:, 0:1] == x.astype(F32)
        second = col[:, 1:2] == x.astype(F32)
        where = jnp.where(first, col[:, 2:3], jnp.where(second, col[:, 3:4], -1.0))
        weight = jnp.where(first, col[:, 4:5], jnp.where(second, col[:, 5:6], 0.0))
        slot = lax.broadcasted_iota(jnp.int32, (tokens, cap), 1).astype(F32)
        pick = (where == slot).astype(F32).astype(BF16)
        acc[...] += weight * jnp.dot(pick, ref[m], preferred_element_type=F32)

    sharing = QH // KVH

    def attend(b, half):
        base = pl.multiple_of(b * WINDOW, WINDOW)
        qi = lax.broadcasted_iota(jnp.int32, (WINDOW, 2 * WINDOW), 0)
        kj = lax.broadcasted_iota(jnp.int32, (WINDOW, 2 * WINDOW), 1)
        dist = qi + WINDOW - kj
        seen = (dist >= 0) & (dist < WINDOW) & (lin * length + base + kj - WINDOW >= 0)
        for pair in range(half * QH // 4, (half + 1) * QH // 4):
            h = 2 * pair // sharing
            lo = (h // 2) * 128
            keys = kvj[0, pl.ds(base, 2 * WINDOW), lo : lo + 128]
            vals = kvj[1, pl.ds(base, 2 * WINDOW), lo : lo + 128]
            off = (h % 2) * HD
            keys = keys[:, off : off + HD]
            vals = vals[:, off : off + HD]
            qp = q[pl.ds(base, WINDOW), pair * 128 : (pair + 1) * 128]
            outs = []
            for g in range(2):
                s = lax.dot_general(
                    qp[:, g * HD : (g + 1) * HD], keys, (((1,), (1,)), ((), ())),
                    preferred_element_type=F32,
                ) * HD ** (-0.5)
                s = jnp.where(seen, s, -1e30)
                sink = sink_ref[2 * pair + g]
                top = jnp.maximum(jnp.max(s, axis=1, keepdims=True), sink)
                w = jnp.exp(s - top)
                tot = jnp.sum(w, axis=1, keepdims=True) + jnp.exp(sink - top)
                o = jnp.dot(w.astype(BF16), vals, preferred_element_type=F32)
                outs.append((o / tot).astype(BF16))
            att_ref[pl.ds(base, WINDOW), pair * 128 : (pair + 1) * 128] = jnp.concatenate(outs, axis=1)

    order = [0, *range(1, near - 1), *range(near, n), near - 1]

    def chosen(i):
        m = order[0]
        for j in range(1, n):
            m = jnp.where(i >= j, order[j], m)
        return m

    blocks = length // WINDOW
    units = 2 * blocks

    def pass_on(g, r):
        m = g * near + r
        S[m] = gathered(slots_of(g, partner(r)), raw[g])
        send_rows(m)

    def take_raw(g):
        m = g * near
        with jax.named_scope("w_raw"):
            expect(posm.at[g], pos_r.at[g])
            expect(raw.at[g], raw_r.at[g])
        with jax.named_scope("relay_rows"):
            for r in range(1, near - 1):
                pass_on(g, r)
            X[m, own] = gathered(slots_of(g, e), raw[g])
            spread(X, m, x_s, x2)

    def take(i):
        m = chosen(i)

        @pl.when((i < n) & (m >= wide) & (lax.rem(m, near) != 0))
        def _():
            with jax.named_scope("w_r1"):
                expect(X.at[m, own], r1.at[m])
            spread(X, m, x_s, x2)

    def fill(i):
        m = chosen(i)

        @pl.when((i < n) & (m >= wide))
        def _():
            with jax.named_scope("w_x2"):
                expect(X.at[m, pl.ds(0, ny - 1)], x2.at[m])
            relay(X, m, x_s, x3)

        @pl.when((i < n) & (m < wide))
        def _():
            with jax.named_scope("w_r1n"):
                expect(X.at[m, pl.ds(0, ny)], r1.at[m])
            relay(X, m, x_s, x3)

    loads[0].wait()
    loads[1].wait()

    def when_raw(i, mark):
        for g in range(1, sides):
            @pl.when(i == near * (g - 1) + mark)
            def _(g=g):
                take_raw(g)

    early = lax.rem(e // (near // 2), 2) == lax.rem(e // near, 2)

    def unit(u, _):
        for half in range(2):
            @pl.when(lax.rem(u, 2) == half)
            def _(half=half):
                with jax.named_scope("attend"):
                    attend(blocks - 1 - u // 2, half)
        return 0

    def share(j):
        m = chosen(j)
        with jax.named_scope("w_h2"):
            expect(H.at[m, pl.ds(0, ny - 1)], h2.at[m])
        relay(H, m, h_s, h3)

    def compute(j, _):
        m = chosen(j)

        @pl.when(j == n - 1)
        def _():
            fill(j)

        @pl.when(j > 0)
        def _():
            with jax.named_scope("w_x3"):
                expect(X.at[m, pl.ds(0, ny)], x3.at[m])

        with jax.named_scope("gate_up"):
            gate_up(m)
        spread(H, m, h_s, h2)
        return 0

    def finish(j, _):
        m = chosen(j)
        with jax.named_scope("w_h3"):
            expect(H.at[m, pl.ds(0, ny)], h3.at[m])
        with jax.named_scope("down"):
            down(m)

        @pl.when(j > 0)
        def _():
            pltpu.make_async_remote_copy(
                src_ref=O.at[m], dst_ref=R.at[m], send_sem=o_s.at[m], recv_sem=o_r.at[m],
                device_id=(partner(m), t), device_id_type=MESH,
            ).start()

        @pl.when(j == 0)
        def _():
            combine(m, O)

        return 0

    def step(i, _):
        @pl.when(early)
        def _():
            when_raw(i, RAWAT)

        @pl.when(i >= near - 1)
        def _():
            take(i + 1)

        for g in range(1, sides):
            @pl.when(i == near * g - 1)
            def _(g=g):
                pass_on(g, near - 1)

        @pl.when((i == near - 1) & jnp.logical_not(early))
        def _():
            share(i - 1)

        @pl.when((i > 0) & (i < n - 1))
        def _():
            fill(i)

        lax.fori_loop(jnp.where(i > n - 2, n, i), jnp.where(i >= n - 2, n, i + 1), compute, 0)

        @pl.when(i == 0)
        def _():
            for c in loads[2:]:
                c.wait()
            details[4].wait()
            lax.fori_loop(0, units - 2, unit, 0)

        @pl.when(jnp.logical_not(early))
        def _():
            when_raw(i, RAWAT)

        @pl.when((i == 0) | (i == 2) | ((i == near - 1) & early) | ((i >= near) & (i - 1 < n)))
        def _():
            share(jnp.where(i == 0, 0, i - 1))

        lax.fori_loop(
            jnp.where(i <= near, jnp.maximum(i - 2, 0), jnp.minimum(i - 1, n)),
            jnp.where(i < near, i - 1, jnp.minimum(i, n)), finish, 0,
        )

        @pl.when(i == n)
        def _():
            @pl.when(lin > 0)
            def _():
                with jax.named_scope("w_edge"):
                    edge.wait_recv()

            lax.fori_loop(units - 2, units, unit, 0)

        @pl.when(i == 3)
        def _():
            send_near(near - 1)

        @pl.when((i > LAG) & (i - LAG < n))
        def _():
            m = chosen(i - LAG)
            with jax.named_scope("w_o"):
                expect(R.at[m], o_r.at[m])
            with jax.named_scope("combine"):
                combine(m, R)

        return 0

    lax.fori_loop(0, n + LAG, step, 0)
    mix_ref[...] = acc[...].astype(BF16)

    def drain(m, _):
        @pl.when(m >= wide)
        def _():
            @pl.when(lax.rem(m, near) > 0)
            def _():
                expect(S.at[m], s_s.at[m])

            expect(X.at[m, pl.ds(0, 2 * ny - 1)], x_s.at[m])

        @pl.when((m > 0) & (m < wide))
        def _():
            expect(SN.at[m], s_s.at[m])
            expect(X.at[m, pl.ds(0, ny)], x_s.at[m])

        @pl.when(m > 0)
        def _():
            expect(O.at[m], o_s.at[m])

        @pl.when((m > 0) & (m < sides))
        def _():
            expect(posm.at[m], pos_s.at[m])
            expect(raw.at[m], raw_s.at[m])

        expect(H.at[m, pl.ds(0, 2 * ny - 1)], h_s.at[m])
        return 0

    with jax.named_scope("drain"):
        lax.fori_loop(0, n, drain, 0)

    @pl.when(lin < total - 1)
    def _():
        edge.wait_send()


def shards(
    queries, keys_values, sink_logits, moe_rows, norm_gain, group_choice, member_choice,
    route_weight, w_gate, w_up, w_down,
):
    n = lax.axis_size("ep")
    tp = lax.axis_size("tp")
    assert w_gate.shape[0] == 1
    tokens, width = moe_rows.shape
    cap = 2 * TOP * tokens // n
    ffs = w_gate.shape[2]
    out = w_down.shape[2]
    ff = w_down.shape[1]
    length = queries.shape[0]
    vmem = pl.BlockSpec(memory_space=pltpu.VMEM)
    anyspace = pl.BlockSpec(memory_space=pl.ANY)
    dma = pltpu.SemaphoreType.DMA
    return pl.pallas_call(
        functools.partial(kernel, n, tp, cap),
        out_shape=(
            pltpu.VMEM(queries.shape, BF16),
            pltpu.VMEM((tokens, out), BF16),
        ),
        in_specs=[
            anyspace, anyspace, anyspace, anyspace, anyspace, anyspace, anyspace, anyspace,
            anyspace, anyspace, anyspace,
        ],
        out_specs=(vmem, vmem),
        scratch_shapes=[
            pltpu.VMEM((width, ffs), BF16),
            pltpu.VMEM((width, ffs), BF16),
            pltpu.VMEM((ff, out), BF16),
            pltpu.VMEM(queries.shape, BF16),
            pltpu.VMEM(moe_rows.shape, BF16),
            pltpu.SMEM(sink_logits.shape, F32),
            pltpu.VMEM((1, width), F32),
            pltpu.VMEM((1, tokens), jnp.int32),
            pltpu.VMEM((TOP, tokens), jnp.int32),
            pltpu.VMEM((TOP, tokens), F32),
            pltpu.VMEM((2, WINDOW + length, keys_values.shape[2]), BF16),
            pltpu.VMEM((tp, tokens, width // tp), BF16),
            pltpu.VMEM((n // min(EPG, n), tokens, width // tp), BF16),
            pltpu.VMEM((n // min(EPG, n), n, tokens), jnp.int32),
            pltpu.VMEM((n, cap, width // tp), BF16),
            pltpu.VMEM((min(EPG, n), tp // CORES, cap, width // tp), BF16),
            pltpu.VMEM((n, tp, cap, width // tp), BF16),
            pltpu.VMEM((n, tp, cap, ffs), BF16),
            pltpu.VMEM((n, cap, out), BF16),
            pltpu.VMEM((n, cap, out), BF16),
            pltpu.VMEM((tokens, out), F32),
            pltpu.VMEM((128, tokens), F32),
            pltpu.VMEM((tokens, 128), F32),
            dma((5,)), dma((5 + ROW_PARTS,)), dma, dma,
            dma((n // min(EPG, n),)), dma((n // min(EPG, n),)), dma((n // min(EPG, n),)), dma((n // min(EPG, n),)),
            dma((n,)), dma((n,)), dma((n,)), dma((n,)), dma((n,)),
            dma((n,)), dma((n,)), dma((n,)), dma((n,)), dma((n,)),
        ],
        compiler_params=pltpu.CompilerParams(
            collective_id=0, has_side_effects=True, vmem_limit_bytes=56 * 1024 * 1024
        ),
    )(
        queries, keys_values, sink_logits, moe_rows, norm_gain.reshape(1, width),
        group_choice.reshape(1, tokens), member_choice.T, route_weight.T, w_gate, w_up, w_down,
    )


def solution(mesh):
    in_specs = (
        P(("ep", "tp"), None),
        P(None, ("ep", "tp"), None),
        P(),
        P("ep", None),
        P(),
        P("ep"),
        P("ep", None),
        P("ep", None),
        P("ep", None, "tp"),
        P("ep", None, "tp"),
        P("ep", None, "tp"),
    )
    out_specs = (P(("ep", "tp"), None), P("ep", "tp"))
    return jax.shard_map(shards, mesh=mesh, in_specs=in_specs, out_specs=out_specs, check_vma=False)
```

```python
import functools

import jax
import jax.numpy as jnp
from jax import lax
from jax.experimental import pallas as pl
from jax.experimental.pallas import tpu as pltpu
from jax.sharding import PartitionSpec as P

QH = 16
KVH = 4
HD = 64
WINDOW = 128
EPG = 4
TOP = 2
CORES = 2
ROW_PARTS = 4
WIDE = 4
RAWAT = 2
LAG = 6
MESH = pl.DeviceIdType.MESH
F32 = jnp.float32
BF16 = jnp.bfloat16


def kernel(
    n, tp, cap,
    q_hbm, kv_hbm, sink_hbm, rows_hbm, gain_hbm, group_hbm, member_hbm, rw_hbm,
    wg_hbm, wu_hbm, wd_hbm,
    att_ref, mix_ref,
    wg, wu, wd, q, rows, sink_ref, gain_ref, group_ref, member_ref, rw_ref, kvj, nrm, raw, posm, S, SN, X, H, O, R, acc, line, col,
    small, loc, edge_s, edge_r, raw_s, raw_r, pos_s, pos_r, s_s, r1, x_s, x2, x3, h_s, h2, h3, o_s, o_r,
):
    e = lax.axis_index("ep")
    t = lax.axis_index("tp")
    ny = tp // CORES
    y = t // CORES
    core = lax.rem(t, CORES)
    mate = y * CORES + (1 - core)
    near = min(EPG, n)
    sides = n // near
    wide = min(WIDE, near)
    tokens, width = rows.shape
    dc = width // tp
    ffs = wg.shape[1]
    length = q.shape[0]
    lin = e * tp + t
    total = n * tp
    after = lax.rem(lin + 1, total)
    before = lax.rem(lin + total - 1, total)
    home = core * ny
    own = home + y

    def block_of(k):
        return (k % CORES) * ny + k // CORES

    def partner(m):
        out = 0
        bit = 1
        while bit < n:
            out = out + bit * lax.rem(e // bit + m // bit, 2)
            bit *= 2
        return out

    def ypeer(j):
        return lax.rem(y + j, ny) * CORES + core

    barrier = pltpu.get_barrier_semaphore()

    def greet(m, _):
        pl.semaphore_signal(barrier, inc=1, device_id=(partner(m), t), device_id_type=MESH)
        return 0

    lax.fori_loop(1, near, greet, 0)
    lax.fori_loop(1, sides, lambda g, _: greet(g * near, _), 0)
    for j in range(1, ny):
        pl.semaphore_signal(barrier, inc=1, device_id=(e, ypeer(j)), device_id_type=MESH)
    pl.semaphore_signal(barrier, inc=1, device_id=(e, mate), device_id_type=MESH)

    @pl.when(lin > 0)
    def _():
        pl.semaphore_signal(
            barrier, inc=1, device_id=(before // tp, lax.rem(before, tp)), device_id_type=MESH
        )

    part = tokens // ROW_PARTS

    def row_load(k):
        at = pl.ds(k * part, part)
        return pltpu.make_async_copy(rows_hbm.at[at], rows.at[at], loc.at[k])

    row_loads = [row_load(k) for k in range(ROW_PARTS)]
    loads = [
        pltpu.make_async_copy(wg_hbm.at[0], wg, loc.at[ROW_PARTS + 0]),
        pltpu.make_async_copy(wu_hbm.at[0], wu, loc.at[ROW_PARTS + 1]),
        pltpu.make_async_copy(q_hbm, q, loc.at[ROW_PARTS + 2]),
        pltpu.make_async_copy(kv_hbm, kvj.at[:, pl.ds(WINDOW, length)], loc.at[ROW_PARTS + 3]),
        pltpu.make_async_copy(wd_hbm.at[0], wd, loc.at[ROW_PARTS + 4]),
    ]
    details = [
        pltpu.make_async_copy(a, b, small.at[i])
        for i, (a, b) in enumerate([
            (group_hbm, group_ref), (member_hbm, member_ref), (rw_hbm, rw_ref),
            (gain_hbm, gain_ref), (sink_hbm, sink_ref),
        ])
    ]
    for c in details[:3] + row_loads + details[3:]:
        c.start()

    for c in details[:3]:
        c.wait()
    a_i = lax.broadcasted_iota(jnp.int32, (tokens, tokens), 0)
    b_i = lax.broadcasted_iota(jnp.int32, (tokens, tokens), 1)
    erow = lax.broadcasted_iota(jnp.int32, (n, tokens), 0)
    e0 = group_ref[...] * EPG + member_ref[0:1, :]
    e1 = group_ref[...] * EPG + member_ref[1:2, :]
    named = (e0 == erow) | (e1 == erow)
    upper = (a_i < b_i).astype(F32).astype(BF16)
    pos = jnp.dot(named.astype(F32).astype(BF16), upper, preferred_element_type=F32)
    posm[0] = jnp.where(named, pos, -1.0).astype(jnp.int32)
    line[0:1, :] = e0.astype(F32)
    line[1:2, :] = e1.astype(F32)
    line[2:3, :] = jnp.sum(jnp.where(e0 == erow, pos, 0.0), axis=0, keepdims=True)
    line[3:4, :] = jnp.sum(jnp.where(e1 == erow, pos, 0.0), axis=0, keepdims=True)
    line[4:6, :] = rw_ref[...]
    line[6:, :] = jnp.zeros((122, tokens), F32)
    col[...] = line[...].T
    acc[...] = jnp.zeros_like(acc)

    @pl.when(lin == 0)
    def _():
        kvj[:, 0:WINDOW, :] = jnp.zeros((2, WINDOW, kvj.shape[2]), BF16)

    chunk = 32

    def norm_rows(r, _):
        at = pl.ds(pl.multiple_of(r * chunk, chunk), chunk)
        v = rows[at, :].astype(F32)
        m = jnp.mean(v * v, axis=1, keepdims=True)
        nv = (v * lax.rsqrt(m + 1e-06) * gain_ref[...]).astype(BF16)
        for k in range(tp):
            nrm[block_of(k), at, :] = nv[:, k * dc : (k + 1) * dc]
        return 0

    details[3].wait()
    for k in range(ROW_PARTS):
        row_loads[k].wait()
        if k == ROW_PARTS - 1:
            for c in loads:
                c.start()
        with jax.named_scope("norm"):
            lax.fori_loop(k * part // chunk, (k + 1) * part // chunk, norm_rows, 0, unroll=2)

    def slots_of(side, x):
        slot = lax.broadcasted_iota(jnp.int32, (cap, tokens), 0)
        return (posm[side, pl.ds(x, 1), :] == slot).astype(F32).astype(BF16)

    def gathered(slots, rows_of):
        return jnp.dot(slots, rows_of, preferred_element_type=F32).astype(BF16)

    edge = pltpu.make_async_remote_copy(
        src_ref=kv_hbm.at[:, pl.ds(length - WINDOW, WINDOW)], dst_ref=kvj.at[:, pl.ds(0, WINDOW)],
        send_sem=edge_s, recv_sem=edge_r,
        device_id=(after // tp, lax.rem(after, tp)), device_id_type=MESH,
    )

    def send_rows(m):
        pltpu.make_async_remote_copy(
            src_ref=S.at[m], dst_ref=X.at[m, own], send_sem=s_s.at[m], recv_sem=r1.at[m],
            device_id=(partner(lax.rem(m, near)), t), device_id_type=MESH,
        ).start()

    def send_near(m):
        slots = slots_of(0, partner(m))
        if m < wide:
            for j in range(ny):
                SN[m, j] = gathered(slots, nrm[home + j])
            pltpu.make_async_remote_copy(
                src_ref=SN.at[m], dst_ref=X.at[m, pl.ds(home, ny)], send_sem=s_s.at[m],
                recv_sem=r1.at[m], device_id=(partner(m), t), device_id_type=MESH,
            ).start()
        else:
            S[m] = gathered(slots, nrm[own])
            send_rows(m)

    def send_raw(g, _):
        to = (partner(g * near), t)
        pltpu.make_async_remote_copy(
            src_ref=posm.at[0], dst_ref=posm.at[g], send_sem=pos_s.at[g], recv_sem=pos_r.at[g],
            device_id=to, device_id_type=MESH,
        ).start()
        pltpu.make_async_remote_copy(
            src_ref=nrm.at[own], dst_ref=raw.at[g], send_sem=raw_s.at[g], recv_sem=raw_r.at[g],
            device_id=to, device_id_type=MESH,
        ).start()
        return 0

    with jax.named_scope("barrier"):
        greeted = (near - 1) + (sides - 1) + (ny - 1) + 1
        pl.semaphore_wait(barrier, jnp.where(lin < total - 1, greeted + 1, greeted))
    with jax.named_scope("build"):
        first_near = near // 2
        send_near(first_near)
        lax.fori_loop(1, sides, send_raw, 0)
        for m in range(1, near - 1):
            if m != first_near:
                send_near(m)

    @pl.when(lin < total - 1)
    def _():
        edge.start()

    mine = slots_of(0, e)
    for k in range(tp):
        X[0, k] = gathered(mine, nrm[k])

    def expect(ref, sem):
        pltpu.make_async_copy(ref, ref, sem).wait()

    def spread(buf, m, sends, to_y):
        for j in range(1, ny):
            pltpu.make_async_remote_copy(
                src_ref=buf.at[m, own], dst_ref=buf.at[m, own], send_sem=sends.at[m],
                recv_sem=to_y.at[m], device_id=(e, ypeer(j)), device_id_type=MESH,
            ).start()

    def relay(buf, m, sends, to_mate):
        half = buf.at[m, pl.ds(home, ny)]
        pltpu.make_async_remote_copy(
            src_ref=half, dst_ref=half, send_sem=sends.at[m],
            recv_sem=to_mate.at[m], device_id=(e, mate), device_id_type=MESH,
        ).start()

    def gate_up(m):
        x = jnp.concatenate([X[m, block_of(k)] for k in range(tp)], axis=1)
        step = min(256, ffs)
        for c in range(0, ffs, step):
            g = jnp.dot(x, wg[:, c : c + step], preferred_element_type=F32)
            u = jnp.dot(x, wu[:, c : c + step], preferred_element_type=F32)
            H[m, own, :, c : c + step] = (g / (1.0 + jnp.exp(-g)) * u).astype(BF16)

    def down(m):
        h = jnp.concatenate([H[m, block_of(k)] for k in range(tp)], axis=1)
        O[m] = jnp.dot(h, wd[...], preferred_element_type=F32).astype(BF16)

    def combine(m, ref):
        x = partner(m)
        first = col[:, 0:1] == x.astype(F32)
        second = col[:, 1:2] == x.astype(F32)
        where = jnp.where(first, col[:, 2:3], jnp.where(second, col[:, 3:4], -1.0))
        weight = jnp.where(first, col[:, 4:5], jnp.where(second, col[:, 5:6], 0.0))
        slot = lax.broadcasted_iota(jnp.int32, (tokens, cap), 1).astype(F32)
        pick = (where == slot).astype(F32).astype(BF16)
        acc[...] += weight * jnp.dot(pick, ref[m], preferred_element_type=F32)

    sharing = QH // KVH

    def attend(b, half):
        base = pl.multiple_of(b * WINDOW, WINDOW)
        qi = lax.broadcasted_iota(jnp.int32, (WINDOW, 2 * WINDOW), 0)
        kj = lax.broadcasted_iota(jnp.int32, (WINDOW, 2 * WINDOW), 1)
        dist = qi + WINDOW - kj
        seen = (dist >= 0) & (dist < WINDOW) & (lin * length + base + kj - WINDOW >= 0)
        for pair in range(half * QH // 4, (half + 1) * QH // 4):
            h = 2 * pair // sharing
            lo = (h // 2) * 128
            keys = kvj[0, pl.ds(base, 2 * WINDOW), lo : lo + 128]
            vals = kvj[1, pl.ds(base, 2 * WINDOW), lo : lo + 128]
            off = (h % 2) * HD
            keys = keys[:, off : off + HD]
            vals = vals[:, off : off + HD]
            qp = q[pl.ds(base, WINDOW), pair * 128 : (pair + 1) * 128]
            outs = []
            for g in range(2):
                s = lax.dot_general(
                    qp[:, g * HD : (g + 1) * HD], keys, (((1,), (1,)), ((), ())),
                    preferred_element_type=F32,
                ) * HD ** (-0.5)
                s = jnp.where(seen, s, -1e30)
                sink = sink_ref[2 * pair + g]
                top = jnp.maximum(jnp.max(s, axis=1, keepdims=True), sink)
                w = jnp.exp(s - top)
                tot = jnp.sum(w, axis=1, keepdims=True) + jnp.exp(sink - top)
                o = jnp.dot(w.astype(BF16), vals, preferred_element_type=F32)
                outs.append((o / tot).astype(BF16))
            att_ref[pl.ds(base, WINDOW), pair * 128 : (pair + 1) * 128] = jnp.concatenate(outs, axis=1)

    order = [0, *range(1, near - 1), *range(near, n), near - 1]

    def chosen(i):
        m = order[0]
        for j in range(1, n):
            m = jnp.where(i >= j, order[j], m)
        return m

    blocks = length // WINDOW
    units = 2 * blocks

    def pass_on(g, r):
        m = g * near + r
        S[m] = gathered(slots_of(g, partner(r)), raw[g])
        send_rows(m)

    def take_raw(g):
        m = g * near
        with jax.named_scope("w_raw"):
            expect(posm.at[g], pos_r.at[g])
            expect(raw.at[g], raw_r.at[g])
        with jax.named_scope("relay_rows"):
            for r in range(1, near - 1):
                pass_on(g, r)
            X[m, own] = gathered(slots_of(g, e), raw[g])
            spread(X, m, x_s, x2)

    def take(i):
        m = chosen(i)

        @pl.when((i < n) & (m >= wide) & (lax.rem(m, near) != 0))
        def _():
            with jax.named_scope("w_r1"):
                expect(X.at[m, own], r1.at[m])
            spread(X, m, x_s, x2)

    def fill(i):
        m = chosen(i)

        @pl.when((i < n) & (m >= wide))
        def _():
            with jax.named_scope("w_x2"):
                expect(X.at[m, pl.ds(0, ny - 1)], x2.at[m])
            relay(X, m, x_s, x3)

        @pl.when((i < n) & (m < wide))
        def _():
            with jax.named_scope("w_r1n"):
                expect(X.at[m, pl.ds(0, ny)], r1.at[m])
            relay(X, m, x_s, x3)

    loads[0].wait()
    loads[1].wait()

    def when_raw(i, mark):
        for g in range(1, sides):
            @pl.when(i == near * (g - 1) + mark)
            def _(g=g):
                take_raw(g)

    early = lin >= 0

    def unit(u, _):
        for half in range(2):
            @pl.when(lax.rem(u, 2) == half)
            def _(half=half):
                with jax.named_scope("attend"):
                    attend(blocks - 1 - u // 2, half)
        return 0

    def share(j):
        m = chosen(j)
        with jax.named_scope("w_h2"):
            expect(H.at[m, pl.ds(0, ny - 1)], h2.at[m])
        relay(H, m, h_s, h3)

    def compute(j, _):
        m = chosen(j)

        @pl.when(j == n - 1)
        def _():
            fill(j)

        @pl.when(j > 0)
        def _():
            with jax.named_scope("w_x3"):
                expect(X.at[m, pl.ds(0, ny)], x3.at[m])

        with jax.named_scope("gate_up"):
            gate_up(m)
        spread(H, m, h_s, h2)
        return 0

    def finish(j, _):
        m = chosen(j)
        with jax.named_scope("w_h3"):
            expect(H.at[m, pl.ds(0, ny)], h3.at[m])
        with jax.named_scope("down"):
            down(m)

        @pl.when(j > 0)
        def _():
            pltpu.make_async_remote_copy(
                src_ref=O.at[m], dst_ref=R.at[m], send_sem=o_s.at[m], recv_sem=o_r.at[m],
                device_id=(partner(m), t), device_id_type=MESH,
            ).start()

        @pl.when(j == 0)
        def _():
            combine(m, O)

        return 0

    def step(i, _):
        @pl.when(early)
        def _():
            when_raw(i, RAWAT)

        @pl.when(i >= near - 1)
        def _():
            take(i + 1)

        for g in range(1, sides):
            @pl.when(i == near * g - 1)
            def _(g=g):
                pass_on(g, near - 1)

        @pl.when((i == near - 1) & jnp.logical_not(early))
        def _():
            share(i - 1)

        @pl.when((i > 0) & (i < n - 1))
        def _():
            fill(i)

        lax.fori_loop(i, jnp.where(i > n - 2, i, i + 1), compute, 0)

        @pl.when(i == 0)
        def _():
            for c in loads[2:]:
                c.wait()
            details[4].wait()
            lax.fori_loop(0, units - 2, unit, 0)

        @pl.when(jnp.logical_not(early))
        def _():
            when_raw(i, RAWAT)

        @pl.when(i == near)
        def _():
            finish(i - 2, 0)

        @pl.when((i == 0) | (i == 2) | ((i == near - 1) & early) | ((i >= near) & (i - 1 < n)))
        def _():
            share(jnp.where(i == 0, 0, i - 1))

        lax.fori_loop(jnp.where(i == n - 2, n - 1, n), n, compute, 0)

        lax.fori_loop(
            jnp.where(i < near, jnp.maximum(i - 2, 0), jnp.minimum(i - 1, n)),
            jnp.where(i < near, i - 1, jnp.minimum(i, n)), finish, 0,
        )

        @pl.when(i == n)
        def _():
            @pl.when(lin > 0)
            def _():
                with jax.named_scope("w_edge"):
                    edge.wait_recv()

            lax.fori_loop(units - 2, units, unit, 0)

        @pl.when(i == 3)
        def _():
            send_near(near - 1)

        @pl.when((i > LAG) & (i - LAG < n))
        def _():
            m = chosen(i - LAG)
            with jax.named_scope("w_o"):
                expect(R.at[m], o_r.at[m])
            with jax.named_scope("combine"):
                combine(m, R)

        return 0

    lax.fori_loop(0, n + LAG, step, 0)
    mix_ref[...] = acc[...].astype(BF16)

    def drain(m, _):
        @pl.when(m >= wide)
        def _():
            @pl.when(lax.rem(m, near) > 0)
            def _():
                expect(S.at[m], s_s.at[m])

            expect(X.at[m, pl.ds(0, 2 * ny - 1)], x_s.at[m])

        @pl.when((m > 0) & (m < wide))
        def _():
            expect(SN.at[m], s_s.at[m])
            expect(X.at[m, pl.ds(0, ny)], x_s.at[m])

        @pl.when(m > 0)
        def _():
            expect(O.at[m], o_s.at[m])

        @pl.when((m > 0) & (m < sides))
        def _():
            expect(posm.at[m], pos_s.at[m])
            expect(raw.at[m], raw_s.at[m])

        expect(H.at[m, pl.ds(0, 2 * ny - 1)], h_s.at[m])
        return 0

    with jax.named_scope("drain"):
        lax.fori_loop(0, n, drain, 0)

    @pl.when(lin < total - 1)
    def _():
        edge.wait_send()


def shards(
    queries, keys_values, sink_logits, moe_rows, norm_gain, group_choice, member_choice,
    route_weight, w_gate, w_up, w_down,
):
    n = lax.axis_size("ep")
    tp = lax.axis_size("tp")
    assert w_gate.shape[0] == 1
    tokens, width = moe_rows.shape
    cap = 2 * TOP * tokens // n
    ffs = w_gate.shape[2]
    out = w_down.shape[2]
    ff = w_down.shape[1]
    length = queries.shape[0]
    vmem = pl.BlockSpec(memory_space=pltpu.VMEM)
    anyspace = pl.BlockSpec(memory_space=pl.ANY)
    dma = pltpu.SemaphoreType.DMA
    return pl.pallas_call(
        functools.partial(kernel, n, tp, cap),
        out_shape=(
            pltpu.VMEM(queries.shape, BF16),
            pltpu.VMEM((tokens, out), BF16),
        ),
        in_specs=[
            anyspace, anyspace, anyspace, anyspace, anyspace, anyspace, anyspace, anyspace,
            anyspace, anyspace, anyspace,
        ],
        out_specs=(vmem, vmem),
        scratch_shapes=[
            pltpu.VMEM((width, ffs), BF16),
            pltpu.VMEM((width, ffs), BF16),
            pltpu.VMEM((ff, out), BF16),
            pltpu.VMEM(queries.shape, BF16),
            pltpu.VMEM(moe_rows.shape, BF16),
            pltpu.SMEM(sink_logits.shape, F32),
            pltpu.VMEM((1, width), F32),
            pltpu.VMEM((1, tokens), jnp.int32),
            pltpu.VMEM((TOP, tokens), jnp.int32),
            pltpu.VMEM((TOP, tokens), F32),
            pltpu.VMEM((2, WINDOW + length, keys_values.shape[2]), BF16),
            pltpu.VMEM((tp, tokens, width // tp), BF16),
            pltpu.VMEM((n // min(EPG, n), tokens, width // tp), BF16),
            pltpu.VMEM((n // min(EPG, n), n, tokens), jnp.int32),
            pltpu.VMEM((n, cap, width // tp), BF16),
            pltpu.VMEM((min(EPG, n), tp // CORES, cap, width // tp), BF16),
            pltpu.VMEM((n, tp, cap, width // tp), BF16),
            pltpu.VMEM((n, tp, cap, ffs), BF16),
            pltpu.VMEM((n, cap, out), BF16),
            pltpu.VMEM((n, cap, out), BF16),
            pltpu.VMEM((tokens, out), F32),
            pltpu.VMEM((128, tokens), F32),
            pltpu.VMEM((tokens, 128), F32),
            dma((5,)), dma((5 + ROW_PARTS,)), dma, dma,
            dma((n // min(EPG, n),)), dma((n // min(EPG, n),)), dma((n // min(EPG, n),)), dma((n // min(EPG, n),)),
            dma((n,)), dma((n,)), dma((n,)), dma((n,)), dma((n,)),
            dma((n,)), dma((n,)), dma((n,)), dma((n,)), dma((n,)),
        ],
        compiler_params=pltpu.CompilerParams(
            collective_id=0, has_side_effects=True, vmem_limit_bytes=56 * 1024 * 1024
        ),
    )(
        queries, keys_values, sink_logits, moe_rows, norm_gain.reshape(1, width),
        group_choice.reshape(1, tokens), member_choice.T, route_weight.T, w_gate, w_up, w_down,
    )


def solution(mesh):
    in_specs = (
        P(("ep", "tp"), None),
        P(None, ("ep", "tp"), None),
        P(),
        P("ep", None),
        P(),
        P("ep"),
        P("ep", None),
        P("ep", None),
        P("ep", None, "tp"),
        P("ep", None, "tp"),
        P("ep", None, "tp"),
    )
    out_specs = (P(("ep", "tp"), None), P("ep", "tp"))
    return jax.shard_map(shards, mesh=mesh, in_specs=in_specs, out_specs=out_specs, check_vma=False)
```
